32 devices in a mesh: grp: 2 (over x), ep: 16 (over z, y, core).
Axes of the slice: x: 2, y: 2, z: 4, core: 2. Of those that a mesh axis runs over, the one named last changes fastest.
Arguments:
- tokens: bfloat16 [256, 2048], P(('grp', 'ep')), parts along dimension 0, may hold values from -6 to 6
- routes: int32 [256, 4], P(('grp', 'ep')), parts along dimension 0, may hold values from 0 to 15, all different within a row; in each aligned block of 8 rows (0 to 7, 8 to 15, ...) at most 4 rows name the same one
- gate_weights: float32 [256, 4], P(('grp', 'ep')), parts along dimension 0, may hold values from 0.1 to 1
- norm_gain: float32 [2048], replicated, may hold values from 0.1 to 1.9
- final_gain: float32 [2048], replicated, may hold values from 0.1 to 1.9
- w_gate: bfloat16 [16, 2048, 512], P('ep'), may hold values from -0.088388348 to 0.088388348
- w_up: bfloat16 [16, 2048, 512], P('ep'), may hold values from -0.088388348 to 0.088388348
- w_down: bfloat16 [16, 512, 2048], P('ep'), may hold values from -0.176776695 to 0.176776695
Outputs:
- mixed: bfloat16 [256, 2048], P('grp', 'ep'), parts along dimension 0
The draws below stay inside these ranges and needn't reach their ends.
There are 2 independent parts, one for each index of `grp`. The reference program is written for one: setup_inputs(seed, part) draws one part's arguments, and reference() takes and returns one part's arrays. A program takes and returns all parts, laid end to end along the dimension named above; an argument that names none is the same for every part. Nothing has to cross between parts.
Inputs may be any that keep to these rules, and one draw needn't show every extreme that they name: `routes`: each row names 4 different experts; among the rows of one device no expert is named by more than 4 rows, and some expert reaches 4.
All inputs are finite; a program needn't handle non-finite values.
Results may differ from the reference program's by a relative error of at most 0.008.
Values may be sent and summed in bfloat16 or wider, within the bound.
A program may use at most 64 MiB of HBM per device.

```python
import math
import jax
import jax.numpy as jnp
import numpy as np
from jax import lax

D = 2048
FF_E = 512
TOPK = 4
TOK_DEV = 8
MOST = 4
EXPERTS = 16
TOKENS = 128
N_EP = 16


def shared_experts(key, salt, rows, cols):
    share = 0.5
    common = jax.random.normal(jax.random.fold_in(key, salt), (rows, cols), jnp.float32)
    own = jax.random.normal(jax.random.fold_in(key, salt + 1), (EXPERTS, rows, cols), jnp.float32)
    mixture = math.sqrt(share) * common[None] + math.sqrt(1.0 - share) * own
    return (jnp.clip(mixture, -4.0, 4.0) * rows ** (-0.5)).astype(jnp.bfloat16)


def draw_w_gate(key, part):
    return shared_experts(key, 101, D, FF_E)


def draw_w_up(key, part):
    return shared_experts(key, 203, D, FF_E)


def draw_w_down(key, part):
    return shared_experts(key, 307, FF_E, D)


def level_of(stream_key, dims, split, smallest, top_value):
    def one(axis_at, shards_of):
        heights = jax.random.uniform(jax.random.fold_in(jax.random.fold_in(stream_key, 6), axis_at), (shards_of,), jnp.float32, smallest / len(split), top_value / len(split))
        return jnp.repeat(jnp.exp(heights), dims[axis_at] // shards_of).reshape((-1,) + (1,) * (len(dims) - axis_at - 1))

    factor_of = one(*split[0])
    for cut in split[1:]:
        factor_of = factor_of * one(*cut)
    return factor_of


def deal_out(key, own, number, rows, number_of, top, bound, slope):
    order = jax.random.permutation(key, number_of)
    heavy_load, ordinary = portions_of(number_of, rows * top, bound, slope, True), portions_of(number_of, rows * top, bound, slope, False)
    places = jnp.arange(number_of)

    def named(sizes, offset_by):
        used = int((sizes > 0).sum())
        fixed = max(1, used // 4)
        moved = fixed + (places - fixed + offset_by * (used - fixed)) % max(1, number_of - fixed)
        return jnp.zeros((number_of,), jnp.int32).at[order[jnp.where(places < fixed, places, moved)]].set(jnp.asarray(sizes, jnp.int32))

    sizes = jnp.where(number % 4 == 0, named(heavy_load, number // 4), named(ordinary, number - number // 4 - 1))
    mixed = jax.random.permutation(jax.random.fold_in(own, 3), number_of)
    source_of, sink = mixed[0:number_of // 2 * 2:2], mixed[1:number_of // 2 * 2:2]
    margin = jnp.minimum(sizes[source_of] - 1, bound - sizes[sink]) // 2
    margin = jnp.where((source_of == order[0]) | (sink == order[0]) | (sizes[sink] == 0), 0, jnp.maximum(margin, 0))
    moved = jax.random.randint(jax.random.fold_in(own, 4), (number_of // 2,), 0, 1 << 20) % (margin + 1)
    sizes = sizes.at[source_of].add(-moved).at[sink].add(moved)
    members = jnp.searchsorted(jnp.cumsum(sizes), jnp.arange(rows * top), side="right").astype(jnp.int32)
    table = members.reshape(top, rows).T
    table = table[jax.random.permutation(jax.random.fold_in(own, 1), rows)]
    offset_by = jax.random.randint(jax.random.fold_in(own, 2), (rows, 1), 0, top)
    return jnp.take_along_axis(table, (jnp.arange(top)[None, :] + offset_by) % top, axis=1)


def portions_of(count, total, bound, slope, full):
    portions = [(1 << 20) // math.isqrt(grade ** slope) + 1 for grade in range(1, count + 1)]
    largest = bound if full else min(bound, max(-(-total // count), total * portions[0] // sum(portions)))
    least = 1 if total - largest >= count - 1 else 0
    holding, surplus = [largest] + [least] * (count - 1), total - largest - least * (count - 1)
    while surplus > 0:
        candidates = [i for i in range(1, count) if holding[i] < largest] or [i for i in range(1, count) if holding[i] < bound]
        mass, left = sum([portions[i] for i in candidates]), surplus
        for i in candidates:
            extra = min(bound - holding[i], max(1, left * portions[i] // mass), surplus)
            holding[i] = holding[i] + extra
            surplus = surplus - extra
    return np.array(holding)


def scatter_about(rng, dims, scale, reach, shards=(), held_as=jnp.bfloat16):
    drawn = scale * jax.random.normal(rng, dims, jnp.float32)
    if shards:
        drawn = drawn * level_of(rng, dims, shards, -0.22, 0.18)
    return jnp.clip(drawn, -reach, reach).astype(held_as)


def setup_inputs(seed: int = 0, part: int = 0) -> dict:
    arg_keys = jax.random.split(jax.random.key(seed), 9)
    own_keys = jax.random.split(jax.random.fold_in(arg_keys[8], part), 9)
    tokens = scatter_about(own_keys[0], (TOKENS, D), 1.0, 6.0, ((0, 16),))
    routes_keys = jax.random.split(jax.random.fold_in(own_keys[1], 1), TOKENS // TOK_DEV)
    routes_turns = jax.random.permutation(jax.random.fold_in(own_keys[1], 3), TOKENS // TOK_DEV)
    routes = jax.vmap(lambda own, number: deal_out(jax.random.fold_in(own_keys[1], 2), own, number, TOK_DEV, EXPERTS, TOPK, MOST, 2))(routes_keys, routes_turns).reshape((TOKENS, TOPK))
    gate_weights = jnp.clip(0.1 + 0.9 * jax.random.uniform(own_keys[2], (TOKENS, TOPK), jnp.float32) ** level_of(own_keys[2], (TOKENS, TOPK), ((0, 16),), -0.2, 0.2), 0.1, 1.0)
    norm_gain = jnp.clip(1.0 + 0.18 * jax.random.normal(arg_keys[3], (D,), jnp.float32), 0.1, 1.9)
    final_gain = jnp.clip(1.0 + 0.18 * jax.random.normal(arg_keys[4], (D,), jnp.float32), 0.1, 1.9)
    w_gate = draw_w_gate(jax.random.fold_in(arg_keys[8], 71), part)
    w_up = draw_w_up(jax.random.fold_in(arg_keys[8], 71), part)
    w_down = draw_w_down(jax.random.fold_in(arg_keys[8], 71), part)
    return dict(tokens=tokens, routes=routes, gate_weights=gate_weights, norm_gain=norm_gain, final_gain=final_gain, w_gate=w_gate, w_up=w_up, w_down=w_down)


def reference(tokens, routes, gate_weights, norm_gain, final_gain, w_gate, w_up, w_down):
    epsilon = 1e-06
    values = tokens.astype(jnp.float32)
    normed = (values * lax.rsqrt(lax.optimization_barrier(jnp.mean(values * values, axis=1, keepdims=True)) + epsilon) * norm_gain).astype(jnp.bfloat16)
    capacity = min(TOKENS, N_EP * MOST)
    normed_wide = normed.astype(jnp.float32)

    def one_expert(carry, expert):
        match = (routes == expert).astype(jnp.float32)
        weight_row = lax.optimization_barrier(jnp.sum(match * gate_weights, axis=1))
        used = lax.optimization_barrier(jnp.sum(match, axis=1)).astype(jnp.int32)
        picked = jnp.argsort(1 - used, stable=True)[:capacity].astype(jnp.int32)
        rows = normed_wide[picked]
        gate_mat = lax.dynamic_index_in_dim(w_gate, expert, 0, keepdims=False).astype(jnp.float32)
        up_mat = lax.dynamic_index_in_dim(w_up, expert, 0, keepdims=False).astype(jnp.float32)
        down_mat = lax.dynamic_index_in_dim(w_down, expert, 0, keepdims=False).astype(jnp.float32)
        gate_val = jnp.dot(rows, gate_mat, preferred_element_type=jnp.float32)
        up_val = jnp.dot(rows, up_mat, preferred_element_type=jnp.float32)
        act = (jax.nn.silu(gate_val) * up_val).astype(jnp.bfloat16).astype(jnp.float32)
        result = jnp.dot(act, down_mat, preferred_element_type=jnp.float32).astype(jnp.bfloat16)
        carry = carry.at[picked].add(weight_row[picked][:, None] * result.astype(jnp.float32))
        return (carry, 0)
    start = jnp.zeros((TOKENS, D), jnp.float32)
    combined, unused = lax.scan(one_expert, start, jnp.arange(EXPERTS, dtype=jnp.int32))
    scale = lax.rsqrt(lax.optimization_barrier(jnp.mean(combined * combined, axis=1, keepdims=True)) + epsilon)
    return (combined * scale * final_gain).astype(jnp.bfloat16)
```

```python
import functools

import jax
import jax.numpy as jnp
from jax import lax
from jax.experimental import pallas as pl
from jax.experimental.pallas import tpu as pltpu
from jax.sharding import PartitionSpec as P

MESH = pl.DeviceIdType.MESH
BF16 = jnp.bfloat16
F32 = jnp.float32
NT = (((1,), (1,)), ((), ()))


def each(count, step):
    if count <= 16:
        for i in range(count):
            step(i)
    else:
        lax.fori_loop(0, count, lambda i, c: (step(i), c)[1], 0)


def far_first(i, n):
    half = (i + 1) // 2
    return n // 2 + half * (2 * (i % 2) - 1) * -1


def kernel(n, most, chunks, group, tokens, routes, gates, ngain, fgain, wg, wu, wd, out,
           wg_v, wu_v, wd_v, slots, recv, gate_own, gate_all, act_v, y_v, back, mix, sums_own, sums,
           w_sem, d_sem, s_send, s_recv, g_send, g_recv, y_send, y_recv, q_send, q_recv):
    me = lax.axis_index("ep")
    rows, width = tokens.shape
    topk = routes.shape[1]
    lanes = n * most
    part = width // chunks
    cols = width // n
    total = n * rows
    eps = 1e-06

    def peer(i):
        return lax.rem(me + far_first(i, n), n)

    def weight_copies(k):
        span = pl.ds(k * part, part)
        return (pltpu.make_async_copy(wg.at[0, span], wg_v.at[span], w_sem.at[k]),
                pltpu.make_async_copy(wu.at[0, span], wu_v.at[span], w_sem.at[chunks + k]))

    down_copy = pltpu.make_async_copy(wd.at[0], wd_v, d_sem)

    barrier = pltpu.get_barrier_semaphore()
    each(n - 1, lambda i: pl.semaphore_signal(barrier, inc=1, device_id={"ep": peer(i)}, device_id_type=MESH))
    for k in range(chunks):
        for c in weight_copies(k):
            c.start()
    down_copy.start()

    lane = lax.broadcasted_iota(jnp.int32, (rows, lanes), 1)
    lane_e, lane_c = lane // most, lane % most
    used = jnp.zeros((rows, lanes), F32)
    gate_of = jnp.zeros((rows, lanes), F32)
    for k in range(topk):
        hit = (routes[:, k:k + 1] == lane_e).astype(F32)
        used += hit
        gate_of += hit * gates[:, k:k + 1]
    row_a = lax.broadcasted_iota(jnp.int32, (rows, rows), 0)
    row_b = lax.broadcasted_iota(jnp.int32, (rows, rows), 1)
    before = jnp.dot((row_b < row_a).astype(F32), used, preferred_element_type=F32)
    select = jnp.where(before == lane_c.astype(F32), used, 0.0)
    weight = select * gate_of
    high = weight.astype(BF16)
    low = (weight - high.astype(F32)).astype(BF16)
    gate_own[...] = jnp.concatenate([high, low], axis=1)
    gate_all[me] = gate_own[...]

    values = tokens[...].astype(F32)
    normed = (values * lax.rsqrt(jnp.mean(values * values, axis=1, keepdims=True) + eps) * ngain[...]).astype(BF16)
    pick = jnp.transpose(select).astype(BF16)
    for k in range(chunks):
        sent = jnp.dot(pick, normed[:, k * part:(k + 1) * part], preferred_element_type=F32).astype(BF16)
        sent = sent.reshape(n, most, part)
        slots[k] = sent
        recv[k, me] = slots[k, me]

    pl.semaphore_wait(barrier, n - 1)
    for k in range(chunks):
        def dispatch(i, k=k):
            d = peer(i)
            pltpu.make_async_remote_copy(
                src_ref=slots.at[k, d], dst_ref=recv.at[k, me], send_sem=s_send.at[k], recv_sem=s_recv.at[k],
                device_id={"ep": d}, device_id_type=MESH).start()
        each(n - 1, dispatch)

    def share_gates(i):
        pltpu.make_async_remote_copy(
            src_ref=gate_own, dst_ref=gate_all.at[me], send_sem=g_send, recv_sem=g_recv,
            device_id={"ep": peer(i)}, device_id_type=MESH).start()
    each(n - 1, share_gates)

    def wait_bytes(ref, sem):
        pltpu.make_async_copy(ref, ref, sem).wait()

    gate_val = jnp.zeros((lanes, wg.shape[2]), F32)
    up_val = jnp.zeros((lanes, wg.shape[2]), F32)
    for k in range(chunks):
        for c in weight_copies(k):
            c.wait()
        wait_bytes(recv.at[k, pl.ds(0, n - 1)], s_recv.at[k])
        x = recv[k].reshape(lanes, part)
        gate_val += jnp.dot(x, wg_v[k * part:(k + 1) * part, :], preferred_element_type=F32)
        up_val += jnp.dot(x, wu_v[k * part:(k + 1) * part, :], preferred_element_type=F32)
    act_v[...] = (jax.nn.silu(gate_val) * up_val).astype(BF16)

    down_copy.wait()
    per = group // cols
    n_groups = width // group
    my_group = me // per

    def down(i):
        g = lax.rem(my_group + (far_first(i, n_groups) if n_groups > 1 else 0), n_groups)
        return g

    def project(g, own):
        y = jnp.dot(act_v[...], wd_v[:, pl.ds(pl.multiple_of(g * group, group), group)],
                    preferred_element_type=F32).astype(BF16)
        for j in range(per):
            d = g * per + j
            y_v[d] = y[:, j * cols:(j + 1) * cols]

            def send(d=d):
                pltpu.make_async_remote_copy(
                    src_ref=y_v.at[d], dst_ref=back.at[me], send_sem=y_send, recv_sem=y_recv,
                    device_id={"ep": d}, device_id_type=MESH).start()
            if own:
                pl.when(d != me)(send)
            else:
                send()
    each(n_groups - 1, lambda i: project(lax.rem(my_group + far_first(i, n_groups), n_groups), False))
    project(my_group, True)
    back[me] = y_v[me]

    wait_bytes(gate_all.at[pl.ds(0, n - 1)], g_recv)
    table = gate_all[...].reshape(total, 2 * lanes)
    tile = max(1, 256 // lanes) * lanes
    per_tile = tile // lanes

    def build(i):
        r = lax.broadcasted_iota(jnp.int32, (lanes, tile), 0)
        q = lax.broadcasted_iota(jnp.int32, (lanes, tile), 1)
        spread = (r == (i * per_tile + q // lanes) * most + q % most).astype(BF16)
        t = lax.broadcasted_iota(jnp.int32, (total, tile), 0)
        q2 = lax.broadcasted_iota(jnp.int32, (total, tile), 1)
        mine = (q2 % lanes) // most == t // rows
        for h in range(2):
            w = jnp.dot(table[:, h * lanes:(h + 1) * lanes], spread, preferred_element_type=F32)
            mix[i, h * total:(h + 1) * total] = jnp.where(mine, w, 0.0).astype(BF16)
    each(n // per_tile, build)

    wait_bytes(back.at[pl.ds(0, n - 1)], y_recv)
    both = jnp.zeros((2 * total, cols), F32)

    def gather(i, both):
        r = back[pl.ds(i * per_tile, per_tile)].reshape(tile, cols)
        return both + jnp.dot(mix[i], r, preferred_element_type=F32)
    if n <= 16:
        for i in range(n // per_tile):
            both = gather(i, both)
    else:
        both = lax.fori_loop(0, n // per_tile, gather, both)
    combined = both[:total] + both[total:]

    square = combined * combined
    ones = jnp.ones((8, cols), BF16)
    row = jnp.zeros((8, total), F32)
    for _ in range(3):
        piece = square.astype(BF16)
        row += lax.dot_general(ones, piece, NT, preferred_element_type=F32)
        square = square - piece.astype(F32)
    sums_own[...] = row[:1]
    sums[me] = sums_own[...]

    def share_sums(i):
        pltpu.make_async_remote_copy(
            src_ref=sums_own, dst_ref=sums.at[me], send_sem=q_send, recv_sem=q_recv,
            device_id={"ep": peer(i)}, device_id_type=MESH).start()
    each(n - 1, share_sums)

    per_lane = 128 // cols if cols < 128 else 1
    wide = cols * per_lane
    gain = fgain[:, pl.ds(pl.multiple_of((me // per_lane) * wide, wide), wide)]
    if per_lane > 1:
        gain = functools.reduce(jnp.add, [
            jnp.where(lax.rem(me, per_lane) == j, gain[:, j * cols:(j + 1) * cols], 0.0) for j in range(per_lane)])

    wait_bytes(sums.at[pl.ds(0, n - 1)], q_recv)
    mean = jnp.sum(sums[...], axis=0) * (1.0 / width)
    scale = jnp.transpose(jnp.broadcast_to(lax.rsqrt(mean + eps), (128, total)))
    out[...] = (combined * scale[:, :1] * gain).astype(BF16)

    for k in range(chunks):
        wait_bytes(slots.at[k, pl.ds(0, n - 1)], s_send.at[k])
    wait_bytes(gate_all.at[pl.ds(0, n - 1)], g_send)
    wait_bytes(y_v.at[pl.ds(0, n - 1)], y_send)
    wait_bytes(sums.at[pl.ds(0, n - 1)], q_send)


def shards(tokens, routes, gate_weights, norm_gain, final_gain, w_gate, w_up, w_down):
    n = lax.axis_size("ep")
    rows, width = tokens.shape
    topk = routes.shape[1]
    ff = w_gate.shape[2]
    most = max(2, (2 * rows * topk + n - 1) // n)
    lanes = n * most
    chunks = 4
    cols = width // n
    group = max(256, cols)
    total = n * rows
    tile = max(1, 256 // lanes) * lanes
    vmem = pl.BlockSpec(memory_space=pltpu.VMEM)
    hbm = pl.BlockSpec(memory_space=pl.ANY)
    dma = pltpu.SemaphoreType.DMA
    return pl.pallas_call(
        functools.partial(kernel, n, most, chunks, group),
        out_shape=jax.ShapeDtypeStruct((total, cols), BF16),
        in_specs=[vmem] * 5 + [hbm] * 3,
        out_specs=vmem,
        scratch_shapes=[
            pltpu.VMEM((width, ff), BF16),
            pltpu.VMEM((width, ff), BF16),
            pltpu.VMEM((ff, width), BF16),
            pltpu.VMEM((chunks, n, most, width // chunks), BF16),
            pltpu.VMEM((chunks, n, most, width // chunks), BF16),
            pltpu.VMEM((rows, 2 * lanes), BF16),
            pltpu.VMEM((n, rows, 2 * lanes), BF16),
            pltpu.VMEM((lanes, ff), BF16),
            pltpu.VMEM((n, lanes, cols), BF16),
            pltpu.VMEM((n, lanes, cols), BF16),
            pltpu.VMEM((n * lanes // tile, 2 * total, tile), BF16),
            pltpu.VMEM((1, total), F32),
            pltpu.VMEM((n, 1, total), F32),
            dma((2 * chunks,)), dma, dma((chunks,)), dma((chunks,)),
            dma, dma, dma, dma, dma, dma,
        ],
        compiler_params=pltpu.CompilerParams(collective_id=0, has_side_effects=True, vmem_limit_bytes=56 * 2**20),
    )(tokens, routes, gate_weights, norm_gain.reshape(1, width), final_gain.reshape(1, width), w_gate, w_up, w_down)


def solution(mesh):
    in_specs = (
        P(("grp", "ep"), None),
        P(("grp", "ep"), None),
        P(("grp", "ep"), None),
        P(),
        P(),
        P("ep", None, None),
        P("ep", None, None),
        P("ep", None, None),
    )
    out_specs = P("grp", "ep")
    return jax.shard_map(shards, mesh=mesh, in_specs=in_specs, out_specs=out_specs, check_vma=False)
```

```python
import functools

import jax
import jax.numpy as jnp
from jax import lax
from jax.experimental import pallas as pl
from jax.experimental.pallas import tpu as pltpu
from jax.sharding import PartitionSpec as P

MESH = pl.DeviceIdType.MESH
BF16 = jnp.bfloat16
F32 = jnp.float32
NT = (((1,), (1,)), ((), ()))


def each(count, step):
    if count <= 16:
        for i in range(count):
            step(i)
    else:
        lax.fori_loop(0, count, lambda i, c: (step(i), c)[1], 0)


def far_first(i, n):
    half = (i + 1) // 2
    return n // 2 + half * (2 * (i % 2) - 1) * -1


def kernel(n, most, chunks, group, tokens, routes, gates, ngain, fgain, wg, wu, wd, out,
           wg_v, wu_v, wd_v, slots, recv, gate_own, gate_all, act_v, y_v, back, mix, sums_own, sums,
           w_sem, d_sem, s_send, s_recv, g_send, g_recv, y_send, y_recv, q_send, q_recv):
    me = lax.axis_index("ep")
    rows, width = tokens.shape
    topk = routes.shape[0]
    lanes = n * most
    part = width // chunks
    cols = width // n
    total = n * rows
    eps = 1e-06

    def peer(i):
        return lax.rem(me + far_first(i, n), n)

    def weight_copies(k):
        span = pl.ds(k * part, part)
        return (pltpu.make_async_copy(wg.at[0, span], wg_v.at[span], w_sem.at[k]),
                pltpu.make_async_copy(wu.at[0, span], wu_v.at[span], w_sem.at[chunks + k]))

    down_copy = pltpu.make_async_copy(wd.at[0], wd_v, d_sem)

    barrier = pltpu.get_barrier_semaphore()
    each(n - 1, lambda i: pl.semaphore_signal(barrier, inc=1, device_id={"ep": peer(i)}, device_id_type=MESH))
    for k in range(chunks):
        for c in weight_copies(k):
            c.start()
    down_copy.start()

    slot = lax.broadcasted_iota(jnp.int32, (lanes, rows), 0)
    slot_e, slot_c = slot // most, slot % most
    used = jnp.zeros((lanes, rows), F32)
    gate_of = jnp.zeros((lanes, rows), F32)
    for k in range(topk):
        hit = (routes[k:k + 1, :] == slot_e).astype(F32)
        used += hit
        gate_of += hit * gates[k:k + 1, :]
    row_a = lax.broadcasted_iota(jnp.int32, (rows, rows), 0)
    row_b = lax.broadcasted_iota(jnp.int32, (rows, rows), 1)
    before = jnp.dot(used, (row_a < row_b).astype(F32), preferred_element_type=F32)
    select = jnp.where(before == slot_c.astype(F32), used, 0.0)
    pick = select.astype(BF16)

    values = tokens[...].astype(F32)
    normed = (values * lax.rsqrt(jnp.mean(values * values, axis=1, keepdims=True) + eps) * ngain[...]).astype(BF16)
    for k in range(chunks):
        sent = jnp.dot(pick, normed[:, k * part:(k + 1) * part], preferred_element_type=F32).astype(BF16)
        sent = sent.reshape(n, most, part)
        slots[k] = sent
        recv[k, me] = slots[k, me]
    weight = jnp.transpose(select * gate_of)
    high = weight.astype(BF16)
    low = (weight - high.astype(F32)).astype(BF16)
    gate_own[...] = jnp.concatenate([high, low], axis=1)
    gate_all[me] = gate_own[...]

    pl.semaphore_wait(barrier, n - 1)
    for k in range(chunks):
        def dispatch(i, k=k):
            d = peer(i)
            pltpu.make_async_remote_copy(
                src_ref=slots.at[k, d], dst_ref=recv.at[k, me], send_sem=s_send.at[k], recv_sem=s_recv.at[k],
                device_id={"ep": d}, device_id_type=MESH).start()
        each(n - 1, dispatch)

    def share_gates(i):
        pltpu.make_async_remote_copy(
            src_ref=gate_own, dst_ref=gate_all.at[me], send_sem=g_send, recv_sem=g_recv,
            device_id={"ep": peer(i)}, device_id_type=MESH).start()
    each(n - 1, share_gates)

    def wait_bytes(ref, sem):
        pltpu.make_async_copy(ref, ref, sem).wait()

    gate_val = jnp.zeros((lanes, wg.shape[2]), F32)
    up_val = jnp.zeros((lanes, wg.shape[2]), F32)
    for k in range(chunks):
        for c in weight_copies(k):
            c.wait()
        wait_bytes(recv.at[k, pl.ds(0, n - 1)], s_recv.at[k])
        x = recv[k].reshape(lanes, part)
        gate_val += jnp.dot(x, wg_v[k * part:(k + 1) * part, :], preferred_element_type=F32)
        up_val += jnp.dot(x, wu_v[k * part:(k + 1) * part, :], preferred_element_type=F32)
    act_v[...] = (jax.nn.silu(gate_val) * up_val).astype(BF16)

    down_copy.wait()
    per = group // cols
    n_groups = width // group
    my_group = me // per

    def down(i):
        g = lax.rem(my_group + (far_first(i, n_groups) if n_groups > 1 else 0), n_groups)
        return g

    def project(g, own):
        y = jnp.dot(act_v[...], wd_v[:, pl.ds(pl.multiple_of(g * group, group), group)],
                    preferred_element_type=F32).astype(BF16)
        for j in range(per):
            d = g * per + j
            y_v[d] = y[:, j * cols:(j + 1) * cols]

            def send(d=d):
                pltpu.make_async_remote_copy(
                    src_ref=y_v.at[d], dst_ref=back.at[me], send_sem=y_send, recv_sem=y_recv,
                    device_id={"ep": d}, device_id_type=MESH).start()
            if own:
                pl.when(d != me)(send)
            else:
                send()
    each(n_groups - 1, lambda i: project(lax.rem(my_group + far_first(i, n_groups), n_groups), False))
    project(my_group, True)
    back[me] = y_v[me]

    wait_bytes(gate_all.at[pl.ds(0, n - 1)], g_recv)
    table = gate_all[...].reshape(total, 2 * lanes)
    tile = max(1, 256 // lanes) * lanes
    per_tile = tile // lanes

    def build(i):
        r = lax.broadcasted_iota(jnp.int32, (lanes, tile), 0)
        q = lax.broadcasted_iota(jnp.int32, (lanes, tile), 1)
        spread = (r == (i * per_tile + q // lanes) * most + q % most).astype(BF16)
        t = lax.broadcasted_iota(jnp.int32, (total, tile), 0)
        q2 = lax.broadcasted_iota(jnp.int32, (total, tile), 1)
        mine = (q2 % lanes) // most == t // rows
        for h in range(2):
            w = jnp.dot(table[:, h * lanes:(h + 1) * lanes], spread, preferred_element_type=F32)
            mix[i, h * total:(h + 1) * total] = jnp.where(mine, w, 0.0).astype(BF16)
    each(n // per_tile, build)

    wait_bytes(back.at[pl.ds(0, n - 1)], y_recv)
    both = jnp.zeros((2 * total, cols), F32)

    def gather(i, both):
        r = back[pl.ds(i * per_tile, per_tile)].reshape(tile, cols)
        return both + jnp.dot(mix[i], r, preferred_element_type=F32)
    if n <= 16:
        for i in range(n // per_tile):
            both = gather(i, both)
    else:
        both = lax.fori_loop(0, n // per_tile, gather, both)
    combined = both[:total] + both[total:]

    square = combined * combined
    ones = jnp.ones((8, cols), BF16)
    row = jnp.zeros((8, total), F32)
    for _ in range(3):
        piece = square.astype(BF16)
        row += lax.dot_general(ones, piece, NT, preferred_element_type=F32)
        square = square - piece.astype(F32)
    sums_own[...] = row[:1]
    sums[me] = sums_own[...]

    def share_sums(i):
        pltpu.make_async_remote_copy(
            src_ref=sums_own, dst_ref=sums.at[me], send_sem=q_send, recv_sem=q_recv,
            device_id={"ep": peer(i)}, device_id_type=MESH).start()
    each(n - 1, share_sums)

    per_lane = 128 // cols if cols < 128 else 1
    wide = cols * per_lane
    gain = fgain[:, pl.ds(pl.multiple_of((me // per_lane) * wide, wide), wide)]
    if per_lane > 1:
        gain = functools.reduce(jnp.add, [
            jnp.where(lax.rem(me, per_lane) == j, gain[:, j * cols:(j + 1) * cols], 0.0) for j in range(per_lane)])

    wait_bytes(sums.at[pl.ds(0, n - 1)], q_recv)
    mean = jnp.sum(sums[...], axis=0) * (1.0 / width)
    scale = jnp.transpose(jnp.broadcast_to(lax.rsqrt(mean + eps), (128, total)))
    out[...] = (combined * scale[:, :1] * gain).astype(BF16)

    for k in range(chunks):
        wait_bytes(slots.at[k, pl.ds(0, n - 1)], s_send.at[k])
    wait_bytes(gate_all.at[pl.ds(0, n - 1)], g_send)
    wait_bytes(y_v.at[pl.ds(0, n - 1)], y_send)
    wait_bytes(sums.at[pl.ds(0, n - 1)], q_send)


def shards(tokens, routes, gate_weights, norm_gain, final_gain, w_gate, w_up, w_down):
    n = lax.axis_size("ep")
    rows, width = tokens.shape
    topk = routes.shape[1]
    ff = w_gate.shape[2]
    most = max(2, (2 * rows * topk + n - 1) // n)
    lanes = n * most
    chunks = 4
    cols = width // n
    group = max(256, cols)
    total = n * rows
    tile = max(1, 256 // lanes) * lanes
    vmem = pl.BlockSpec(memory_space=pltpu.VMEM)
    hbm = pl.BlockSpec(memory_space=pl.ANY)
    dma = pltpu.SemaphoreType.DMA
    return pl.pallas_call(
        functools.partial(kernel, n, most, chunks, group),
        out_shape=jax.ShapeDtypeStruct((total, cols), BF16),
        in_specs=[vmem] * 5 + [hbm] * 3,
        out_specs=vmem,
        scratch_shapes=[
            pltpu.VMEM((width, ff), BF16),
            pltpu.VMEM((width, ff), BF16),
            pltpu.VMEM((ff, width), BF16),
            pltpu.VMEM((chunks, n, most, width // chunks), BF16),
            pltpu.VMEM((chunks, n, most, width // chunks), BF16),
            pltpu.VMEM((rows, 2 * lanes), BF16),
            pltpu.VMEM((n, rows, 2 * lanes), BF16),
            pltpu.VMEM((lanes, ff), BF16),
            pltpu.VMEM((n, lanes, cols), BF16),
            pltpu.VMEM((n, lanes, cols), BF16),
            pltpu.VMEM((n * lanes // tile, 2 * total, tile), BF16),
            pltpu.VMEM((1, total), F32),
            pltpu.VMEM((n, 1, total), F32),
            dma((2 * chunks,)), dma, dma((chunks,)), dma((chunks,)),
            dma, dma, dma, dma, dma, dma,
        ],
        compiler_params=pltpu.CompilerParams(collective_id=0, has_side_effects=True, vmem_limit_bytes=56 * 2**20),
    )(tokens, routes.T, gate_weights.T, norm_gain.reshape(1, width), final_gain.reshape(1, width), w_gate, w_up, w_down)


def solution(mesh):
    in_specs = (
        P(("grp", "ep"), None),
        P(("grp", "ep"), None),
        P(("grp", "ep"), None),
        P(),
        P(),
        P("ep", None, None),
        P("ep", None, None),
        P("ep", None, None),
    )
    out_specs = P("grp", "ep")
    return jax.shard_map(shards, mesh=mesh, in_specs=in_specs, out_specs=out_specs, check_vma=False)
```

```python
import functools

import jax
import jax.numpy as jnp
from jax import lax
from jax.experimental import pallas as pl
from jax.experimental.pallas import tpu as pltpu
from jax.sharding import PartitionSpec as P

MESH = pl.DeviceIdType.MESH
BF16 = jnp.bfloat16
F32 = jnp.float32
NT = (((1,), (1,)), ((), ()))


def each(count, step):
    if count <= 16:
        for i in range(count):
            step(i)
    else:
        lax.fori_loop(0, count, lambda i, c: (step(i), c)[1], 0)


def far_first(i, n):
    half = (i + 1) // 2
    return n // 2 + half * (2 * (i % 2) - 1) * -1


def kernel(n, most, chunks, group, tokens_in, routes_in, gates_in, ngain_in, fgain_in, wg, wu, wd, out,
           tokens, routes, gates, ngain, fgain, in_sem,
           wg_v, wu_v, wd_v, slots, recv, gate_own, gate_all, act_v, y_v, back, mix, sums_own, sums,
           w_sem, d_sem, s_send, s_recv, g_send, g_recv, y_send, y_recv, q_send, q_recv):
    me = lax.axis_index("ep")
    rows, width = tokens.shape
    topk = routes.shape[0]
    lanes = n * most
    part = width // chunks
    cols = width // n
    total = n * rows
    eps = 1e-06

    def peer(i):
        return lax.rem(me + far_first(i, n), n)

    def weight_copies(k):
        span = pl.ds(k * part, part)
        return (pltpu.make_async_copy(wg.at[0, span], wg_v.at[span], w_sem.at[k]),
                pltpu.make_async_copy(wu.at[0, span], wu_v.at[span], w_sem.at[chunks + k]))

    down_copy = pltpu.make_async_copy(wd.at[0], wd_v, d_sem)

    barrier = pltpu.get_barrier_semaphore()
    each(n - 1, lambda i: pl.semaphore_signal(barrier, inc=1, device_id={"ep": peer(i)}, device_id_type=MESH))
    small = [pltpu.make_async_copy(a, b, in_sem.at[i]) for i, (a, b) in enumerate((
        (tokens_in, tokens), (routes_in, routes), (gates_in, gates), (ngain_in, ngain), (fgain_in, fgain)))]
    for c in small:
        c.start()
    for k in range(chunks):
        for c in weight_copies(k):
            c.start()
    down_copy.start()
    for c in small:
        c.wait()

    slot = lax.broadcasted_iota(jnp.int32, (lanes, rows), 0)
    slot_e, slot_c = slot // most, slot % most
    used = jnp.zeros((lanes, rows), F32)
    gate_of = jnp.zeros((lanes, rows), F32)
    for k in range(topk):
        hit = (routes[k:k + 1, :] == slot_e).astype(F32)
        used += hit
        gate_of += hit * gates[k:k + 1, :]
    row_a = lax.broadcasted_iota(jnp.int32, (rows, rows), 0)
    row_b = lax.broadcasted_iota(jnp.int32, (rows, rows), 1)
    before = jnp.dot(used, (row_a < row_b).astype(F32), preferred_element_type=F32)
    select = jnp.where(before == slot_c.astype(F32), used, 0.0)
    pick = select.astype(BF16)

    values = tokens[...].astype(F32)
    normed = (values * lax.rsqrt(jnp.mean(values * values, axis=1, keepdims=True) + eps) * ngain[...]).astype(BF16)
    for k in range(chunks):
        sent = jnp.dot(pick, normed[:, k * part:(k + 1) * part], preferred_element_type=F32).astype(BF16)
        sent = sent.reshape(n, most, part)
        slots[k] = sent
        recv[k, me] = slots[k, me]
    weight = jnp.transpose(select * gate_of)
    high = weight.astype(BF16)
    low = (weight - high.astype(F32)).astype(BF16)
    gate_own[...] = jnp.concatenate([high, low], axis=1)
    gate_all[me] = gate_own[...]

    pl.semaphore_wait(barrier, n - 1)
    for k in range(chunks):
        def dispatch(i, k=k):
            d = peer(i)
            pltpu.make_async_remote_copy(
                src_ref=slots.at[k, d], dst_ref=recv.at[k, me], send_sem=s_send.at[k], recv_sem=s_recv.at[k],
                device_id={"ep": d}, device_id_type=MESH).start()
        each(n - 1, dispatch)

    def share_gates(i):
        pltpu.make_async_remote_copy(
            src_ref=gate_own, dst_ref=gate_all.at[me], send_sem=g_send, recv_sem=g_recv,
            device_id={"ep": peer(i)}, device_id_type=MESH).start()
    each(n - 1, share_gates)

    def wait_bytes(ref, sem):
        pltpu.make_async_copy(ref, ref, sem).wait()

    gate_val = jnp.zeros((lanes, wg.shape[2]), F32)
    up_val = jnp.zeros((lanes, wg.shape[2]), F32)
    for k in range(chunks):
        for c in weight_copies(k):
            c.wait()
        wait_bytes(recv.at[k, pl.ds(0, n - 1)], s_recv.at[k])
        x = recv[k].reshape(lanes, part)
        gate_val += jnp.dot(x, wg_v[k * part:(k + 1) * part, :], preferred_element_type=F32)
        up_val += jnp.dot(x, wu_v[k * part:(k + 1) * part, :], preferred_element_type=F32)
    act_v[...] = (jax.nn.silu(gate_val) * up_val).astype(BF16)

    down_copy.wait()
    per = group // cols
    n_groups = width // group
    my_group = me // per

    def down(i):
        g = lax.rem(my_group + (far_first(i, n_groups) if n_groups > 1 else 0), n_groups)
        return g

    def project(g, own):
        y = jnp.dot(act_v[...], wd_v[:, pl.ds(pl.multiple_of(g * group, group), group)],
                    preferred_element_type=F32).astype(BF16)
        for j in range(per):
            d = g * per + j
            y_v[d] = y[:, j * cols:(j + 1) * cols]

            def send(d=d):
                pltpu.make_async_remote_copy(
                    src_ref=y_v.at[d], dst_ref=back.at[me], send_sem=y_send, recv_sem=y_recv,
                    device_id={"ep": d}, device_id_type=MESH).start()
            if own:
                pl.when(d != me)(send)
            else:
                send()
    each(n_groups - 1, lambda i: project(lax.rem(my_group + far_first(i, n_groups), n_groups), False))
    project(my_group, True)
    back[me] = y_v[me]

    wait_bytes(gate_all.at[pl.ds(0, n - 1)], g_recv)
    table = gate_all[...].reshape(total, 2 * lanes)
    tile = max(1, 256 // lanes) * lanes
    per_tile = tile // lanes

    def build(i):
        r = lax.broadcasted_iota(jnp.int32, (lanes, tile), 0)
        q = lax.broadcasted_iota(jnp.int32, (lanes, tile), 1)
        spread = (r == (i * per_tile + q // lanes) * most + q % most).astype(BF16)
        t = lax.broadcasted_iota(jnp.int32, (total, tile), 0)
        q2 = lax.broadcasted_iota(jnp.int32, (total, tile), 1)
        mine = (q2 % lanes) // most == t // rows
        for h in range(2):
            w = jnp.dot(table[:, h * lanes:(h + 1) * lanes], spread, preferred_element_type=F32)
            mix[i, h * total:(h + 1) * total] = jnp.where(mine, w, 0.0).astype(BF16)
    each(n // per_tile, build)

    wait_bytes(back.at[pl.ds(0, n - 1)], y_recv)
    both = jnp.zeros((2 * total, cols), F32)

    def gather(i, both):
        r = back[pl.ds(i * per_tile, per_tile)].reshape(tile, cols)
        return both + jnp.dot(mix[i], r, preferred_element_type=F32)
    if n <= 16:
        for i in range(n // per_tile):
            both = gather(i, both)
    else:
        both = lax.fori_loop(0, n // per_tile, gather, both)
    combined = both[:total] + both[total:]

    square = combined * combined
    ones = jnp.ones((8, cols), BF16)
    row = jnp.zeros((8, total), F32)
    for _ in range(3):
        piece = square.astype(BF16)
        row += lax.dot_general(ones, piece, NT, preferred_element_type=F32)
        square = square - piece.astype(F32)
    sums_own[...] = row[:1]
    sums[me] = sums_own[...]

    def share_sums(i):
        pltpu.make_async_remote_copy(
            src_ref=sums_own, dst_ref=sums.at[me], send_sem=q_send, recv_sem=q_recv,
            device_id={"ep": peer(i)}, device_id_type=MESH).start()
    each(n - 1, share_sums)

    per_lane = 128 // cols if cols < 128 else 1
    wide = cols * per_lane
    gain = fgain[:, pl.ds(pl.multiple_of((me // per_lane) * wide, wide), wide)]
    if per_lane > 1:
        gain = functools.reduce(jnp.add, [
            jnp.where(lax.rem(me, per_lane) == j, gain[:, j * cols:(j + 1) * cols], 0.0) for j in range(per_lane)])

    wait_bytes(sums.at[pl.ds(0, n - 1)], q_recv)
    mean = jnp.sum(sums[...], axis=0) * (1.0 / width)
    scale = jnp.transpose(jnp.broadcast_to(lax.rsqrt(mean + eps), (128, total)))
    out[...] = (combined * scale[:, :1] * gain).astype(BF16)

    for k in range(chunks):
        wait_bytes(slots.at[k, pl.ds(0, n - 1)], s_send.at[k])
    wait_bytes(gate_all.at[pl.ds(0, n - 1)], g_send)
    wait_bytes(y_v.at[pl.ds(0, n - 1)], y_send)
    wait_bytes(sums.at[pl.ds(0, n - 1)], q_send)


def shards(tokens, routes, gate_weights, norm_gain, final_gain, w_gate, w_up, w_down):
    n = lax.axis_size("ep")
    rows, width = tokens.shape
    topk = routes.shape[1]
    ff = w_gate.shape[2]
    most = max(2, (2 * rows * topk + n - 1) // n)
    lanes = n * most
    chunks = 4
    cols = width // n
    group = max(256, cols)
    total = n * rows
    tile = max(1, 256 // lanes) * lanes
    vmem = pl.BlockSpec(memory_space=pltpu.VMEM)
    hbm = pl.BlockSpec(memory_space=pl.ANY)
    dma = pltpu.SemaphoreType.DMA
    return pl.pallas_call(
        functools.partial(kernel, n, most, chunks, group),
        out_shape=jax.ShapeDtypeStruct((total, cols), BF16),
        in_specs=[hbm] * 8,
        out_specs=vmem,
        scratch_shapes=[
            pltpu.VMEM((rows, width), BF16),
            pltpu.VMEM((topk, rows), jnp.int32),
            pltpu.VMEM((topk, rows), F32),
            pltpu.VMEM((1, width), F32),
            pltpu.VMEM((1, width), F32),
            dma((5,)),
            pltpu.VMEM((width, ff), BF16),
            pltpu.VMEM((width, ff), BF16),
            pltpu.VMEM((ff, width), BF16),
            pltpu.VMEM((chunks, n, most, width // chunks), BF16),
            pltpu.VMEM((chunks, n, most, width // chunks), BF16),
            pltpu.VMEM((rows, 2 * lanes), BF16),
            pltpu.VMEM((n, rows, 2 * lanes), BF16),
            pltpu.VMEM((lanes, ff), BF16),
            pltpu.VMEM((n, lanes, cols), BF16),
            pltpu.VMEM((n, lanes, cols), BF16),
            pltpu.VMEM((n * lanes // tile, 2 * total, tile), BF16),
            pltpu.VMEM((1, total), F32),
            pltpu.VMEM((n, 1, total), F32),
            dma((2 * chunks,)), dma, dma((chunks,)), dma((chunks,)),
            dma, dma, dma, dma, dma, dma,
        ],
        compiler_params=pltpu.CompilerParams(collective_id=0, has_side_effects=True, vmem_limit_bytes=56 * 2**20),
    )(tokens, routes.T, gate_weights.T, norm_gain.reshape(1, width), final_gain.reshape(1, width), w_gate, w_up, w_down)


def solution(mesh):
    in_specs = (
        P(("grp", "ep"), None),
        P(("grp", "ep"), None),
        P(("grp", "ep"), None),
        P(),
        P(),
        P("ep", None, None),
        P("ep", None, None),
        P("ep", None, None),
    )
    out_specs = P("grp", "ep")
    return jax.shard_map(shards, mesh=mesh, in_specs=in_specs, out_specs=out_specs, check_vma=False)
```
